128 devices in a mesh: ep: 64 (over z, y, x), tp: 2 (over core).
Axes of the slice: x: 4, y: 4, z: 4, core: 2. Of those that a mesh axis runs over, the one named last changes fastest.
Arguments:
- tokens: bfloat16 [32768, 2048], P(('ep', 'tp')), may hold values from -6 to 6
- norm_gain: float32 [2048], replicated, may hold values from 0.1 to 1.9
- norm_bias: float32 [2048], replicated, may hold values from -3 to 3
- gate_weight: bfloat16 [64, 2048, 1024], P('ep', None, 'tp'), may hold values from -0.125 to 0.125
- up_weight: bfloat16 [64, 2048, 1024], P('ep', None, 'tp'), may hold values from -0.125 to 0.125
- down_weight: bfloat16 [64, 1024, 2048], P('ep', 'tp'), may hold values from -0.1875 to 0.1875
- expert_ids: int32 [32768, 2], P(('ep', 'tp')), may hold values from 0 to 63, all different within a row; in each aligned block of 256 rows (0 to 255, 256 to 511, ...) at most 16 rows name the same one
- route_weights: float32 [32768, 2], P(('ep', 'tp')), may hold values from 0.2 to 1
Outputs:
- mixed: bfloat16 [32768, 2048], P(('ep', 'tp'))
The draws below stay inside these ranges and needn't reach their ends.
Inputs may be any that keep to these rules, and one draw needn't show every extreme that they name: `expert_ids`: a token's 2 experts differ; in the tokens of one device (aligned blocks of 256 rows) no expert is named by more than 16 entries, a bound that some block reaches.
All inputs are finite; a program needn't handle non-finite values.
Results may differ from the reference program's by a relative error of at most 0.0071.
Values may be sent and summed in bfloat16 or wider, within the bound.
No kernel may reach another device: no remote copies, remote signals or barrier semaphores. Data moves between devices by JAX's collectives and lax.ppermute only.
A program may use at most 128 MiB of HBM per device.

```python
import math
import jax
import jax.numpy as jnp
import numpy as np
from jax import lax

D = 2048
FFE = 1024
TOPK = 2
TOK_DEV = 256
EXPERTS = 64
CAP = 16
TOKENS = 32768


def block_scale(key, dims, cuts, least, high):
    def one(dim, shards_of):
        draws = jax.random.uniform(jax.random.fold_in(jax.random.fold_in(key, 6), dim), (shards_of,), jnp.float32, least / len(cuts), high / len(cuts))
        return jnp.repeat(jnp.exp(draws), dims[dim] // shards_of).reshape((-1,) + (1,) * (len(dims) - dim - 1))

    level = one(*cuts[0])
    for cut in cuts[1:]:
        level = level * one(*cut)
    return level


def assign_block(stream_key, own, number, rows, number_of, top, limit, skew):
    ranking = jax.random.permutation(stream_key, number_of)
    heavy_load, common = shares(number_of, rows * top, limit, skew, True), shares(number_of, rows * top, limit, skew, False)
    places = jnp.arange(number_of)

    def named(tallies, offset_by):
        used = int((tallies > 0).sum())
        fixed = max(1, used // 4)
        moved = fixed + (places - fixed + offset_by * (used - fixed)) % max(1, number_of - fixed)
        return jnp.zeros((number_of,), jnp.int32).at[ranking[jnp.where(places < fixed, places, moved)]].set(jnp.asarray(tallies, jnp.int32))

    tallies = jnp.where(number % 4 == 0, named(heavy_load, number // 4), named(common, number - number // 4 - 1))
    mixed = jax.random.permutation(jax.random.fold_in(own, 3), number_of)
    source_of, receiver = mixed[0:number_of // 2 * 2:2], mixed[1:number_of // 2 * 2:2]
    room = jnp.minimum(tallies[source_of] - 1, limit - tallies[receiver]) // 2
    room = jnp.where((source_of == ranking[0]) | (receiver == ranking[0]) | (tallies[receiver] == 0), 0, jnp.maximum(room, 0))
    moved = jax.random.randint(jax.random.fold_in(own, 4), (number_of // 2,), 0, 1 << 20) % (room + 1)
    tallies = tallies.at[source_of].add(-moved).at[receiver].add(moved)
    members = jnp.searchsorted(jnp.cumsum(tallies), jnp.arange(rows * top), side="right").astype(jnp.int32)
    grid = members.reshape(top, rows).T
    grid = grid[jax.random.permutation(jax.random.fold_in(own, 1), rows)]
    offset_by = jax.random.randint(jax.random.fold_in(own, 2), (rows, 1), 0, top)
    return jnp.take_along_axis(grid, (jnp.arange(top)[None, :] + offset_by) % top, axis=1)


def shares(number_of, total, bound, slope, full):
    loads = [(1 << 20) // math.isqrt(rank ** slope) + 1 for rank in range(1, number_of + 1)]
    largest = bound if full else min(bound, max(-(-total // number_of), total * loads[0] // sum(loads)))
    least = 1 if total - largest >= number_of - 1 else 0
    counts, rest = [largest] + [least] * (number_of - 1), total - largest - least * (number_of - 1)
    while rest > 0:
        candidates = [i for i in range(1, number_of) if counts[i] < largest] or [i for i in range(1, number_of) if counts[i] < bound]
        pool, left = sum([loads[i] for i in candidates]), rest
        for i in candidates:
            more = min(bound - counts[i], max(1, left * loads[i] // pool), rest)
            counts[i] = counts[i] + more
            rest = rest - more
    return np.array(counts)


def scatter_about(own_key, shape, width, bound, cuts=(), held_as=jnp.bfloat16):
    array = jax.random.normal(own_key, shape, jnp.float32) * width
    if len(cuts) > 0:
        array = block_scale(own_key, shape, cuts, -0.22, 0.18) * array
    return jnp.clip(array, min=-bound, max=bound).astype(held_as)


def setup_inputs(seed: int = 0) -> dict:
    seeds = jax.random.split(jax.random.key(seed), 9)
    tokens = scatter_about(seeds[0], (TOKENS, D), 1.0, 6.0, ((0, 128),))
    norm_gain = jnp.clip(1.0 + 0.18 * jax.random.normal(seeds[1], (D,), jnp.float32), 0.1, 1.9)
    norm_bias = scatter_about(seeds[2], (D,), 0.5, 3.0, (), jnp.float32)
    gate_weight = scatter_about(seeds[3], (EXPERTS, D, FFE), D ** -0.5, 0.125, ((0, 64), (2, 2)))
    up_weight = scatter_about(seeds[4], (EXPERTS, D, FFE), D ** -0.5, 0.125, ((0, 64), (2, 2)))
    down_weight = scatter_about(seeds[5], (EXPERTS, FFE, D), FFE ** -0.5, 0.1875, ((0, 64), (1, 2)))
    expert_ids_keys = jax.random.split(jax.random.fold_in(seeds[6], 1), TOKENS // TOK_DEV)
    expert_ids_turns = jax.random.permutation(jax.random.fold_in(seeds[6], 3), TOKENS // TOK_DEV)
    expert_ids = jax.vmap(lambda own, number: assign_block(jax.random.fold_in(seeds[6], 2), own, number, TOK_DEV, EXPERTS, TOPK, CAP, 2))(expert_ids_keys, expert_ids_turns).reshape((TOKENS, TOPK))
    route_weights = jnp.clip(0.2 + 0.8 * jax.random.uniform(seeds[7], (TOKENS, TOPK), jnp.float32) ** block_scale(seeds[7], (TOKENS, TOPK), ((0, 128),), -0.2, 0.2), 0.2, 1.0)
    return {"tokens": tokens, "norm_gain": norm_gain, "norm_bias": norm_bias, "gate_weight": gate_weight, "up_weight": up_weight, "down_weight": down_weight, "expert_ids": expert_ids, "route_weights": route_weights}


def expert_rows(rows, w_gate, w_up, w_down):
    gate = jnp.dot(rows, w_gate, preferred_element_type=jnp.float32)
    upper = jnp.dot(rows, w_up, preferred_element_type=jnp.float32)
    hidden = (jax.nn.silu(gate) * upper).astype(jnp.bfloat16)
    return jnp.dot(hidden, w_down, preferred_element_type=jnp.float32).astype(jnp.bfloat16)

def reference(tokens, norm_gain, norm_bias, gate_weight, up_weight, down_weight, expert_ids, route_weights):
    values = tokens.astype(jnp.float32)
    centre = values - lax.optimization_barrier(jnp.mean(values, axis=-1, keepdims=True))
    spread = lax.optimization_barrier(jnp.mean(centre * centre, axis=-1, keepdims=True))
    normed = (centre * lax.rsqrt(spread + 1e-05) * norm_gain + norm_bias).astype(jnp.bfloat16)
    sources = TOKENS // TOK_DEV
    blocks = expert_ids.reshape(sources, TOK_DEV * TOPK)
    onehot = (blocks[:, :, None] == jnp.arange(EXPERTS, dtype=jnp.int32)[None, None, :]).astype(jnp.int32)
    slot = lax.optimization_barrier(jnp.sum(jnp.cumsum(onehot, axis=1) * onehot, axis=-1)) - 1
    row_index = (jnp.arange(sources, dtype=jnp.int32)[:, None] * CAP + slot).reshape(-1).astype(jnp.int32)
    flat_ids = expert_ids.reshape(-1)
    token_rows = jnp.repeat(normed, TOPK, axis=0)
    buffer_rows = sources * CAP

    def one_expert(expert, total):
        chosen = flat_ids == expert
        index = jnp.where(chosen, row_index, buffer_rows).astype(jnp.int32)
        buffer = jnp.zeros((buffer_rows, D), jnp.bfloat16).at[index].set(token_rows, mode='drop')
        result = expert_rows(buffer, gate_weight[expert], up_weight[expert], down_weight[expert])
        picked = result[jnp.minimum(index, buffer_rows - 1)]
        picked = jnp.where(chosen[:, None], picked.astype(jnp.float32), 0.0).reshape(TOKENS, TOPK, D)
        return total + lax.optimization_barrier(jnp.sum(picked * route_weights[:, :, None], axis=1))
    total = lax.fori_loop(0, EXPERTS, one_expert, jnp.zeros((TOKENS, D), jnp.float32))
    return total.astype(jnp.bfloat16)
```

```python
import jax
import jax.numpy as jnp
from jax import lax
from jax.experimental import pallas as pl
from jax.experimental.pallas import tpu as pltpu
from jax.sharding import PartitionSpec as P

BF = jnp.bfloat16
F32 = jnp.float32


def dot(a, b):
    return jnp.dot(a, b, preferred_element_type=F32)


def pack_kernel(experts, capacity, blocks):
    def kernel(tok, gain, bias, ids, ids_t, buf, place, normed, place_t):
        n, width = tok.shape
        rows = experts * capacity // blocks
        step = pl.program_id(0)

        @pl.when(step == 0)
        def _():
            values = tok[...].astype(F32)
            centre = values - jnp.mean(values, axis=-1, keepdims=True)
            spread = jnp.mean(centre * centre, axis=-1, keepdims=True)
            normed[...] = (centre * lax.rsqrt(spread + 1e-05) * gain[...] + bias[...]).astype(BF)
            i = lax.broadcasted_iota(jnp.int32, (n, n), 0)
            j = lax.broadcasted_iota(jnp.int32, (n, n), 1)
            e = lax.broadcasted_iota(jnp.int32, (experts, n), 0)
            one = [(e == ids_t[k : k + 1, :]).astype(F32) for k in range(2)]
            seen = dot((one[0] + one[1]).astype(BF), (i < j).astype(BF))
            for k in range(2):
                slot = jnp.sum(seen * one[k], axis=0, keepdims=True).astype(jnp.int32)
                place_t[k : k + 1, :] = ids_t[k : k + 1, :] * capacity + slot
            e = lax.broadcasted_iota(jnp.int32, (n, experts), 1)
            one = [(e == ids[:, k : k + 1]).astype(F32) for k in range(2)]
            seen = dot((j < i).astype(BF), (one[0] + one[1]).astype(BF))
            for k in range(2):
                slot = jnp.sum(seen * one[k], axis=1, keepdims=True).astype(jnp.int32)
                place[:, k : k + 1] = ids[:, k : k + 1] * capacity + slot

        r = lax.broadcasted_iota(jnp.int32, (rows, n), 0) + step * rows
        hit = (r == place_t[0:1, :]) | (r == place_t[1:2, :])
        buf[...] = dot(jnp.where(hit, 1.0, 0.0).astype(BF), normed[...]).astype(BF)

    return kernel


def pack(tokens, gain, bias, ids, experts, capacity):
    n, width = tokens.shape
    blocks = 4
    whole = lambda s: (0, 0)
    return pl.pallas_call(
        pack_kernel(experts, capacity, blocks),
        grid=(blocks,),
        in_specs=[
            pl.BlockSpec((n, width), whole),
            pl.BlockSpec((1, width), whole),
            pl.BlockSpec((1, width), whole),
            pl.BlockSpec((n, 2), whole),
            pl.BlockSpec((2, n), whole),
        ],
        out_specs=[
            pl.BlockSpec((experts * capacity // blocks, width), lambda s: (s, 0)),
            pl.BlockSpec((n, 2), whole),
        ],
        out_shape=[
            jax.ShapeDtypeStruct((experts * capacity, width), BF),
            jax.ShapeDtypeStruct((n, 2), jnp.int32),
        ],
        scratch_shapes=[pltpu.VMEM((n, width), BF), pltpu.VMEM((2, n), jnp.int32)],
        compiler_params=pltpu.CompilerParams(dimension_semantics=("arbitrary",)),
        name="pack",
    )(tokens, gain.reshape(1, -1), bias.reshape(1, -1), ids, ids.T)


def expert_kernel(x, ga, gb, ua, ub, da, db, out):
    rows = x[...]
    total = None
    for g, u, d in ((ga, ua, da), (gb, ub, db)):
        gate = dot(rows, g[...])
        hidden = (gate / (1.0 + jnp.exp(-gate)) * dot(rows, u[...])).astype(BF)
        part = dot(hidden, d[...])
        total = part if total is None else total + part
    out[...] = total.astype(BF)


def expert(x, weights):
    rows, width = x.shape
    tile = 256
    fixed = [
        pl.BlockSpec(w.shape, lambda s: (0, 0), pipeline_mode=pl.Buffered(1)) for w in weights
    ]
    return pl.pallas_call(
        expert_kernel,
        grid=(rows // tile,),
        in_specs=[pl.BlockSpec((tile, width), lambda s: (s, 0))] + fixed,
        out_specs=pl.BlockSpec((tile, width), lambda s: (s, 0)),
        out_shape=jax.ShapeDtypeStruct((rows, width), BF),
        compiler_params=pltpu.CompilerParams(
            dimension_semantics=("arbitrary",), vmem_limit_bytes=48 * 1024 * 1024
        ),
        name="expert",
    )(x, *weights)


def mix_kernel(ret, place, weight, out, pick):
    n = out.shape[0]
    rows = ret.shape[0]

    @pl.when(pl.program_id(0) == 0)
    def _():
        r = lax.broadcasted_iota(jnp.int32, (n, rows), 1)
        for k in range(2):
            pick[k * n : k * n + n, :] = jnp.where(r == place[:, k : k + 1], 1.0, 0.0).astype(BF)

    picked = dot(pick[...], ret[...])
    out[...] = (picked[:n] * weight[:, 0:1] + picked[n:] * weight[:, 1:2]).astype(BF)


def mix(ret, place, weight):
    rows, width = ret.shape
    n = place.shape[0]
    tile = 512
    return pl.pallas_call(
        mix_kernel,
        grid=(width // tile,),
        in_specs=[
            pl.BlockSpec((rows, tile), lambda s: (0, s)),
            pl.BlockSpec((n, 2), lambda s: (0, 0)),
            pl.BlockSpec((n, 2), lambda s: (0, 0)),
        ],
        out_specs=pl.BlockSpec((n, tile), lambda s: (0, s)),
        out_shape=jax.ShapeDtypeStruct((n, width), BF),
        scratch_shapes=[pltpu.VMEM((2 * n, rows), BF)],
        compiler_params=pltpu.CompilerParams(dimension_semantics=("arbitrary",)),
        name="mix",
    )(ret, place, weight)


def body(
    tokens, norm_gain, norm_bias, gate_weight, up_weight, down_weight, expert_ids, route_weights
):
    tok_rows, width = tokens.shape
    experts = lax.axis_size("ep")
    capacity = max(4 * tok_rows // experts, 4)
    swap = [(0, 1), (1, 0)]
    mine = [gate_weight[0], up_weight[0], down_weight[0]]
    weights = []
    for w in mine:
        weights += [w, lax.ppermute(w, "tp", swap)]
    buffer, place = pack(tokens, norm_gain, norm_bias, expert_ids, experts, capacity)
    rows = lax.all_to_all(
        buffer.reshape(experts, capacity, width), "ep", split_axis=0, concat_axis=0, tiled=True
    )
    result = expert(rows.reshape(-1, width), weights)
    returned = lax.all_to_all(
        result.reshape(experts, capacity, width), "ep", split_axis=0, concat_axis=0, tiled=True
    )
    return mix(returned.reshape(-1, width), place, route_weights)


def solution(mesh):
    placed = (
        P(("ep", "tp"), None),
        P(),
        P(),
        P("ep", None, "tp"),
        P("ep", None, "tp"),
        P("ep", "tp", None),
        P(("ep", "tp"), None),
        P(("ep", "tp"), None),
    )
    return jax.shard_map(
        body, mesh=mesh, in_specs=placed, out_specs=P(("ep", "tp"), None), check_vma=False
    )
```

```python
import jax
import jax.numpy as jnp
from jax import lax
from jax.experimental import pallas as pl
from jax.experimental.pallas import tpu as pltpu
from jax.sharding import PartitionSpec as P


BF = jnp.bfloat16
F32 = jnp.float32


def dot(a, b):
    return jnp.dot(a, b, preferred_element_type=F32)


def place_rows(ids_t, experts, capacity):
    n = ids_t.shape[1]
    i = lax.broadcasted_iota(jnp.int32, (n, n), 0)
    j = lax.broadcasted_iota(jnp.int32, (n, n), 1)
    e = lax.broadcasted_iota(jnp.int32, (experts, n), 0)
    one = [(e == ids_t[k : k + 1, :]).astype(F32) for k in range(2)]
    seen = dot((one[0] + one[1]).astype(BF), (i < j).astype(BF))
    slots = [jnp.sum(seen * o, axis=0, keepdims=True).astype(jnp.int32) for o in one]
    return [ids_t[k : k + 1, :] * capacity + slots[k] for k in range(2)]


def pack_kernel(tok, gain, bias, ids_t, buf):
    n, width = tok.shape
    rows = buf.shape[0]
    experts = rows // CAP
    place = place_rows(ids_t[...], experts, CAP)
    values = tok[...].astype(F32)
    centre = values - jnp.mean(values, axis=-1, keepdims=True)
    spread = jnp.mean(centre * centre, axis=-1, keepdims=True)
    normed = (centre * lax.rsqrt(spread + 1e-05) * gain[...] + bias[...]).astype(BF)
    tile = 256
    for s in range(0, rows, tile):
        r = lax.broadcasted_iota(jnp.int32, (tile, n), 0) + s
        hit = (r == place[0]) | (r == place[1])
        buf[s : s + tile, :] = dot(jnp.where(hit, 1.0, 0.0).astype(BF), normed).astype(BF)


VM = pl.BlockSpec(memory_space=pltpu.VMEM)
CAP = 16
MB = 1024 * 1024


def pack(tokens, gain, bias, ids, rows):
    n, width = tokens.shape
    return pl.pallas_call(
        pack_kernel,
        in_specs=[VM] * 4,
        out_specs=VM,
        out_shape=jax.ShapeDtypeStruct((rows, width), BF),
        compiler_params=pltpu.CompilerParams(vmem_limit_bytes=14 * MB),
        name="pack",
    )(tokens, gain.reshape(1, -1), bias.reshape(1, -1), ids.T)


def expert_kernel(x, ga, gb, ua, ub, da, db, mark, out):
    tile = 256

    def step(i, _):
        at = pl.ds(pl.multiple_of(i * tile, tile), tile)
        rows = x[at, :]
        total = None
        for g, u, d in ((ga, ua, da), (gb, ub, db)):
            gate = dot(rows, g[...])
            hidden = (gate / (1.0 + jnp.exp(-gate)) * dot(rows, u[...])).astype(BF)
            part = dot(hidden, d[...])
            total = part if total is None else total + part
        out[at, :] = total.astype(BF)
        return _

    lax.fori_loop(0, x.shape[0] // tile, step, 0)


def expert(x, weights, mark):
    rows, width = x.shape
    return pl.pallas_call(
        expert_kernel,
        in_specs=[VM] * 8,
        out_specs=VM,
        out_shape=jax.ShapeDtypeStruct((rows, width), BF),
        compiler_params=pltpu.CompilerParams(vmem_limit_bytes=28 * MB),
        name="expert",
    )(x, *weights, mark)


def mix_kernel(ret, ids_t, weight_t, out, side):
    rows = ret.shape[0]
    n, width = out.shape
    place = place_rows(ids_t[...], rows // CAP, CAP)
    side[...] = jnp.zeros(side.shape, F32)
    for k in range(2):
        side[k : k + 1, :] = place[k].astype(F32)
        side[2 + k : 3 + k, :] = weight_t[k : k + 1, :]
    cols = side[...].T
    r = lax.broadcasted_iota(jnp.int32, (n, rows), 1)
    pick = [
        jnp.where(r == cols[:, k : k + 1].astype(jnp.int32), 1.0, 0.0).astype(BF) for k in range(2)
    ]
    tile = 512
    for s in range(0, width, tile):
        part = ret[:, s : s + tile]
        out[:, s : s + tile] = (
            dot(pick[0], part) * cols[:, 2:3] + dot(pick[1], part) * cols[:, 3:4]
        ).astype(BF)


def mix(ret, ids, weight):
    n = ids.shape[0]
    return pl.pallas_call(
        mix_kernel,
        in_specs=[VM] * 3,
        out_specs=VM,
        out_shape=jax.ShapeDtypeStruct((n, ret.shape[1]), BF),
        scratch_shapes=[pltpu.VMEM((8, n), F32)],
        compiler_params=pltpu.CompilerParams(vmem_limit_bytes=14 * MB),
        name="mix",
    )(ret, ids.T, weight.T)


def body(
    tokens, norm_gain, norm_bias, gate_weight, up_weight, down_weight, expert_ids, route_weights
):
    width = tokens.shape[1]
    experts = lax.axis_size("ep")
    swap = [(0, 1), (1, 0)]
    weights = []
    for w in (gate_weight[0], up_weight[0], down_weight[0]):
        weights += [w, lax.ppermute(w, "tp", swap)]
    buffer = pack(tokens, norm_gain, norm_bias, expert_ids, experts * CAP)
    rows = lax.all_to_all(
        buffer.reshape(experts, CAP, width), "ep", split_axis=0, concat_axis=0, tiled=True
    ).reshape(-1, width)
    mark = rows[:16, :128] * 2
    result = expert(rows, weights, mark)
    returned = lax.all_to_all(
        result.reshape(experts, CAP, width), "ep", split_axis=0, concat_axis=0, tiled=True
    )
    return mix(returned.reshape(-1, width), expert_ids, route_weights)


def solution(mesh):
    placed = (
        P(("ep", "tp"), None),
        P(),
        P(),
        P("ep", None, "tp"),
        P("ep", None, "tp"),
        P("ep", "tp", None),
        P(("ep", "tp"), None),
        P(("ep", "tp"), None),
    )
    return jax.shard_map(
        body, mesh=mesh, in_specs=placed, out_specs=P(("ep", "tp"), None), check_vma=False
    )
```

```python
import jax
import jax.numpy as jnp
from jax import lax
from jax.experimental import pallas as pl
from jax.experimental.pallas import tpu as pltpu
from jax.sharding import PartitionSpec as P


BF = jnp.bfloat16
F32 = jnp.float32


def dot(a, b):
    return jnp.dot(a, b, preferred_element_type=F32)


def place_rows(ids_t, experts, capacity):
    n = ids_t.shape[1]
    i = lax.broadcasted_iota(jnp.int32, (n, n), 0)
    j = lax.broadcasted_iota(jnp.int32, (n, n), 1)
    e = lax.broadcasted_iota(jnp.int32, (experts, n), 0)
    one = [(e == ids_t[k : k + 1, :]).astype(F32) for k in range(2)]
    seen = dot((one[0] + one[1]).astype(BF), (i < j).astype(BF))
    slots = [jnp.sum(seen * o, axis=0, keepdims=True).astype(jnp.int32) for o in one]
    return [ids_t[k : k + 1, :] * capacity + slots[k] for k in range(2)]


def stay(a):
    return pltpu.with_memory_space_constraint(a, pltpu.HBM)


def pack_kernel(tok, gain, bias, ids_t, buf, tok_v, gain_v, bias_v, ids_v, normed, sems):
    n, _ = tok.shape
    rows = buf.shape[0]
    part = n // PARTS
    small = [
        pltpu.make_async_copy(src, dst, sems.at[i])
        for i, (src, dst) in enumerate(((ids_t, ids_v), (gain, gain_v), (bias, bias_v)))
    ]
    large = [
        pltpu.make_async_copy(
            tok.at[pl.ds(i * part, part)], tok_v.at[pl.ds(i * part, part)], sems.at[3 + i]
        )
        for i in range(PARTS)
    ]
    for copy in small + large:
        copy.start()
    small[0].wait()
    place = place_rows(ids_v[...], rows // CAP, CAP)
    small[1].wait()
    small[2].wait()
    for i in range(PARTS):
        large[i].wait()
        at = pl.ds(i * part, part)
        values = tok_v[at, :].astype(F32)
        centre = values - jnp.mean(values, axis=-1, keepdims=True)
        spread = jnp.mean(centre * centre, axis=-1, keepdims=True)
        normed[at, :] = (
            centre * lax.rsqrt(spread + 1e-05) * gain_v[...] + bias_v[...]
        ).astype(BF)
    tile = 256
    for s in range(0, rows, tile):
        r = lax.broadcasted_iota(jnp.int32, (tile, n), 0) + s
        hit = (r == place[0]) | (r == place[1])
        buf[s : s + tile, :] = dot(jnp.where(hit, 1.0, 0.0).astype(BF), normed[...]).astype(BF)


PARTS = 4
HB = pl.BlockSpec(memory_space=pltpu.HBM)
VM = pl.BlockSpec(memory_space=pltpu.VMEM)
CAP = 16
MB = 1024 * 1024


def pack(tokens, gain, bias, ids, rows):
    n, width = tokens.shape
    return pl.pallas_call(
        pack_kernel,
        in_specs=[HB] * 4,
        out_specs=VM,
        out_shape=jax.ShapeDtypeStruct((rows, width), BF),
        scratch_shapes=[
            pltpu.VMEM((n, width), BF),
            pltpu.VMEM((1, width), F32),
            pltpu.VMEM((1, width), F32),
            pltpu.VMEM((2, n), jnp.int32),
            pltpu.VMEM((n, width), BF),
            pltpu.SemaphoreType.DMA((3 + PARTS,)),
        ],
        compiler_params=pltpu.CompilerParams(vmem_limit_bytes=14 * MB),
        name="pack",
    )(*[stay(a) for a in (tokens, gain.reshape(1, -1), bias.reshape(1, -1), ids.T)])


def expert_kernel(x, ga, gb, ua, ub, da, db, mark, out):
    tile = 256
    for s in range(0, x.shape[0], tile):
        rows = x[s : s + tile, :]
        total = None
        for g, u, d in ((ga, ua, da), (gb, ub, db)):
            gate = dot(rows, g[...])
            hidden = (gate / (1.0 + jnp.exp(-gate)) * dot(rows, u[...])).astype(BF)
            part = dot(hidden, d[...])
            total = part if total is None else total + part
        out[s : s + tile, :] = total.astype(BF)


def expert(x, weights, mark):
    rows, width = x.shape
    return pl.pallas_call(
        expert_kernel,
        in_specs=[VM] * 8,
        out_specs=VM,
        out_shape=jax.ShapeDtypeStruct((rows, width), BF),
        compiler_params=pltpu.CompilerParams(vmem_limit_bytes=28 * MB),
        name="expert",
    )(x, *weights, mark)


def mix_kernel(ret, ids_t, weight_t, out, side, done, sems):
    rows = ret.shape[0]
    n, width = out.shape
    place = place_rows(ids_t[...], rows // CAP, CAP)
    side[...] = jnp.zeros(side.shape, F32)
    for k in range(2):
        side[k : k + 1, :] = place[k].astype(F32)
        side[2 + k : 3 + k, :] = weight_t[k : k + 1, :]
    cols = side[...].T
    r = lax.broadcasted_iota(jnp.int32, (n, rows), 1)
    pick = [
        jnp.where(r == cols[:, k : k + 1].astype(jnp.int32), 1.0, 0.0).astype(BF) for k in range(2)
    ]
    for i in range(TILES):
        at = pl.ds(i * (width // TILES), width // TILES)
        part = ret[:, at]
        done[:, at] = (
            dot(pick[0], part) * cols[:, 2:3] + dot(pick[1], part) * cols[:, 3:4]
        ).astype(BF)
        pltpu.make_async_copy(done.at[:, at], out.at[:, at], sems.at[i]).start()
    for i in range(TILES):
        at = pl.ds(i * (width // TILES), width // TILES)
        pltpu.make_async_copy(done.at[:, at], out.at[:, at], sems.at[i]).wait()


TILES = 4


def mix(ret, ids, weight):
    n = ids.shape[0]
    return pl.pallas_call(
        mix_kernel,
        in_specs=[VM] * 3,
        out_specs=HB,
        out_shape=jax.ShapeDtypeStruct((n, ret.shape[1]), BF),
        scratch_shapes=[
            pltpu.VMEM((8, n), F32),
            pltpu.VMEM((n, ret.shape[1]), BF),
            pltpu.SemaphoreType.DMA((TILES,)),
        ],
        compiler_params=pltpu.CompilerParams(vmem_limit_bytes=14 * MB),
        name="mix",
    )(ret, ids.T, weight.T)


def body(
    tokens, norm_gain, norm_bias, gate_weight, up_weight, down_weight, expert_ids, route_weights
):
    width = tokens.shape[1]
    experts = lax.axis_size("ep")
    swap = [(0, 1), (1, 0)]
    weights = []
    for w in (gate_weight[0], up_weight[0], down_weight[0]):
        weights += [w, lax.ppermute(w, "tp", swap)]
    buffer = pack(tokens, norm_gain, norm_bias, expert_ids, experts * CAP)
    rows = lax.all_to_all(
        buffer.reshape(experts, CAP, width), "ep", split_axis=0, concat_axis=0, tiled=True
    ).reshape(-1, width)
    mark = rows[:16, :128] * 2
    result = expert(rows, weights, mark)
    returned = lax.all_to_all(
        result.reshape(experts, CAP, width), "ep", split_axis=0, concat_axis=0, tiled=True
    )
    return mix(returned.reshape(-1, width), expert_ids, route_weights)


def solution(mesh):
    placed = (
        P(("ep", "tp"), None),
        P(),
        P(),
        P("ep", None, "tp"),
        P("ep", None, "tp"),
        P("ep", "tp", None),
        P(("ep", "tp"), None),
        P(("ep", "tp"), None),
    )
    return jax.shard_map(
        body, mesh=mesh, in_specs=placed, out_specs=P(("ep", "tp"), None), check_vma=False
    )
```

```python
import jax
import jax.numpy as jnp
from jax import lax
from jax.experimental import pallas as pl
from jax.experimental.pallas import tpu as pltpu
from jax.sharding import PartitionSpec as P


BF = jnp.bfloat16
F32 = jnp.float32


def dot(a, b):
    return jnp.dot(a, b, preferred_element_type=F32)


def place_rows(ids_t, experts, capacity):
    n = ids_t.shape[1]
    i = lax.broadcasted_iota(jnp.int32, (n, n), 0)
    j = lax.broadcasted_iota(jnp.int32, (n, n), 1)
    e = lax.broadcasted_iota(jnp.int32, (experts, n), 0)
    one = [(e == ids_t[k : k + 1, :]).astype(F32) for k in range(2)]
    seen = dot((one[0] + one[1]).astype(BF), (i < j).astype(BF))
    slots = [jnp.sum(seen * o, axis=0, keepdims=True).astype(jnp.int32) for o in one]
    return [ids_t[k : k + 1, :] * capacity + slots[k] for k in range(2)]


def stay(a):
    return pltpu.with_memory_space_constraint(a, pltpu.HBM)


def pack_kernel(tok, gain, bias, ids_t, buf, tok_v, gain_v, bias_v, ids_v, normed, ticks, sems):
    n, _ = tok.shape
    rows = buf.shape[0]
    part = n // PARTS
    small = [
        pltpu.make_async_copy(src, dst, sems.at[i])
        for i, (src, dst) in enumerate(((ids_t, ids_v), (gain, gain_v), (bias, bias_v)))
    ]
    large = [
        pltpu.make_async_copy(
            tok.at[pl.ds(i * part, part)], tok_v.at[pl.ds(i * part, part)], sems.at[3 + i]
        )
        for i in range(PARTS)
    ]
    for copy in small + large:
        copy.start()
    ticks[0] = 0

    def tick(i, carry):
        ticks[0] = ticks[0] + i
        return carry

    lax.fori_loop(0, lax.axis_index("tp") * HOLD, tick, 0)
    small[0].wait()
    place = place_rows(ids_v[...], rows // CAP, CAP)
    small[1].wait()
    small[2].wait()
    for i in range(PARTS):
        large[i].wait()
        at = pl.ds(i * part, part)
        values = tok_v[at, :].astype(F32)
        centre = values - jnp.mean(values, axis=-1, keepdims=True)
        spread = jnp.mean(centre * centre, axis=-1, keepdims=True)
        normed[at, :] = (
            centre * lax.rsqrt(spread + 1e-05) * gain_v[...] + bias_v[...]
        ).astype(BF)
    tile = 256
    for s in range(0, rows, tile):
        r = lax.broadcasted_iota(jnp.int32, (tile, n), 0) + s
        hit = (r == place[0]) | (r == place[1])
        buf[s : s + tile, :] = dot(jnp.where(hit, 1.0, 0.0).astype(BF), normed[...]).astype(BF)


PARTS = 4
HOLD = 3050
HB = pl.BlockSpec(memory_space=pltpu.HBM)
VM = pl.BlockSpec(memory_space=pltpu.VMEM)
CAP = 16
MB = 1024 * 1024


def pack(tokens, gain, bias, ids, rows):
    n, width = tokens.shape
    return pl.pallas_call(
        pack_kernel,
        in_specs=[HB] * 4,
        out_specs=VM,
        out_shape=jax.ShapeDtypeStruct((rows, width), BF),
        scratch_shapes=[
            pltpu.VMEM((n, width), BF),
            pltpu.VMEM((1, width), F32),
            pltpu.VMEM((1, width), F32),
            pltpu.VMEM((2, n), jnp.int32),
            pltpu.VMEM((n, width), BF),
            pltpu.SMEM((1,), jnp.int32),
            pltpu.SemaphoreType.DMA((3 + PARTS,)),
        ],
        compiler_params=pltpu.CompilerParams(vmem_limit_bytes=14 * MB),
        name="pack",
    )(*[stay(a) for a in (tokens, gain.reshape(1, -1), bias.reshape(1, -1), ids.T)])


def expert_kernel(x, ga, gb, ua, ub, da, db, mark, out):
    tile = 256
    for s in range(0, x.shape[0], tile):
        rows = x[s : s + tile, :]
        total = None
        for g, u, d in ((ga, ua, da), (gb, ub, db)):
            gate = dot(rows, g[...])
            hidden = (gate / (1.0 + jnp.exp(-gate)) * dot(rows, u[...])).astype(BF)
            part = dot(hidden, d[...])
            total = part if total is None else total + part
        out[s : s + tile, :] = total.astype(BF)


def expert(x, weights, mark):
    rows, width = x.shape
    return pl.pallas_call(
        expert_kernel,
        in_specs=[VM] * 8,
        out_specs=VM,
        out_shape=jax.ShapeDtypeStruct((rows, width), BF),
        compiler_params=pltpu.CompilerParams(vmem_limit_bytes=28 * MB),
        name="expert",
    )(x, *weights, mark)


def mix_kernel(ret, ids_t, weight_t, out, side, done, sems):
    rows = ret.shape[0]
    n, width = out.shape
    place = place_rows(ids_t[...], rows // CAP, CAP)
    side[...] = jnp.zeros(side.shape, F32)
    for k in range(2):
        side[k : k + 1, :] = place[k].astype(F32)
        side[2 + k : 3 + k, :] = weight_t[k : k + 1, :]
    cols = side[...].T
    r = lax.broadcasted_iota(jnp.int32, (n, rows), 1)
    pick = [
        jnp.where(r == cols[:, k : k + 1].astype(jnp.int32), 1.0, 0.0).astype(BF) for k in range(2)
    ]
    for i in range(TILES):
        at = pl.ds(i * (width // TILES), width // TILES)
        part = ret[:, at]
        done[:, at] = (
            dot(pick[0], part) * cols[:, 2:3] + dot(pick[1], part) * cols[:, 3:4]
        ).astype(BF)
        pltpu.make_async_copy(done.at[:, at], out.at[:, at], sems.at[i]).start()
    for i in range(TILES):
        at = pl.ds(i * (width // TILES), width // TILES)
        pltpu.make_async_copy(done.at[:, at], out.at[:, at], sems.at[i]).wait()


TILES = 4


def mix(ret, ids, weight):
    n = ids.shape[0]
    return pl.pallas_call(
        mix_kernel,
        in_specs=[VM] * 3,
        out_specs=HB,
        out_shape=jax.ShapeDtypeStruct((n, ret.shape[1]), BF),
        scratch_shapes=[
            pltpu.VMEM((8, n), F32),
            pltpu.VMEM((n, ret.shape[1]), BF),
            pltpu.SemaphoreType.DMA((TILES,)),
        ],
        compiler_params=pltpu.CompilerParams(vmem_limit_bytes=14 * MB),
        name="mix",
    )(ret, ids.T, weight.T)


def body(
    tokens, norm_gain, norm_bias, gate_weight, up_weight, down_weight, expert_ids, route_weights
):
    width = tokens.shape[1]
    experts = lax.axis_size("ep")
    swap = [(0, 1), (1, 0)]
    weights = []
    for w in (gate_weight[0], up_weight[0], down_weight[0]):
        weights += [w, lax.ppermute(w, "tp", swap)]
    buffer = pack(tokens, norm_gain, norm_bias, expert_ids, experts * CAP)
    rows = lax.all_to_all(
        buffer.reshape(experts, CAP, width), "ep", split_axis=0, concat_axis=0, tiled=True
    ).reshape(-1, width)
    mark = rows[:16, :128] * 2
    result = expert(rows, weights, mark)
    returned = lax.all_to_all(
        result.reshape(experts, CAP, width), "ep", split_axis=0, concat_axis=0, tiled=True
    )
    return mix(returned.reshape(-1, width), expert_ids, route_weights)


def solution(mesh):
    placed = (
        P(("ep", "tp"), None),
        P(),
        P(),
        P("ep", None, "tp"),
        P("ep", None, "tp"),
        P("ep", "tp", None),
        P(("ep", "tp"), None),
        P(("ep", "tp"), None),
    )
    return jax.shard_map(
        body, mesh=mesh, in_specs=placed, out_specs=P(("ep", "tp"), None), check_vma=False
    )
```

```python
import jax
import jax.numpy as jnp
from jax import lax
from jax.experimental import pallas as pl
from jax.experimental.pallas import tpu as pltpu
from jax.sharding import PartitionSpec as P


BF = jnp.bfloat16
F32 = jnp.float32


def dot(a, b):
    return jnp.dot(a, b, preferred_element_type=F32)


def place_rows(ids_t, experts, capacity):
    n = ids_t.shape[1]
    i = lax.broadcasted_iota(jnp.int32, (n, n), 0)
    j = lax.broadcasted_iota(jnp.int32, (n, n), 1)
    e = lax.broadcasted_iota(jnp.int32, (experts, n), 0)
    one = [(e == ids_t[k : k + 1, :]).astype(F32) for k in range(2)]
    seen = dot((one[0] + one[1]).astype(BF), (i < j).astype(BF))
    slots = [jnp.sum(seen * o, axis=0, keepdims=True).astype(jnp.int32) for o in one]
    return [ids_t[k : k + 1, :] * capacity + slots[k] for k in range(2)]


def picks(place, weight_t, side, pick):
    side[...] = jnp.zeros(side.shape, F32)
    for k in range(2):
        side[k : k + 1, :] = place[k].astype(F32)
        side[2 + k : 3 + k, :] = weight_t[k : k + 1, :]
    cols = side[...].T
    r = lax.broadcasted_iota(jnp.int32, pick.shape, 1)
    hit = [r == cols[:, k : k + 1].astype(jnp.int32) for k in range(2)]
    pick[...] = jnp.where(
        hit[0], cols[:, 2:3], jnp.where(hit[1], cols[:, 3:4], 0.0)
    ).astype(BF)


def stay(a):
    return pltpu.with_memory_space_constraint(a, pltpu.HBM)


def pack_kernel(
    tok, gain, bias, ids_t, weight_t, buf, pick,
    tok_v, gain_v, bias_v, ids_v, weight_v, normed, side, ticks, sems,
):
    n, _ = tok.shape
    rows = buf.shape[0]
    part = n // PARTS
    small = [
        pltpu.make_async_copy(src, dst, sems.at[i])
        for i, (src, dst) in enumerate(
            ((ids_t, ids_v), (gain, gain_v), (bias, bias_v), (weight_t, weight_v))
        )
    ]
    large = [
        pltpu.make_async_copy(
            tok.at[pl.ds(i * part, part)], tok_v.at[pl.ds(i * part, part)], sems.at[4 + i]
        )
        for i in range(PARTS)
    ]
    for copy in small + large:
        copy.start()
    small[0].wait()
    small[3].wait()
    place = place_rows(ids_v[...], rows // CAP, CAP)

    @pl.when(lax.axis_index("tp") == LAST)
    def _():
        picks(place, weight_v, side, pick)
        ticks[0] = 0

        def tick(i, carry):
            ticks[0] = ticks[0] + i
            return carry

        lax.fori_loop(0, HOLD, tick, 0)

    small[1].wait()
    small[2].wait()
    for i in range(PARTS):
        large[i].wait()
        at = pl.ds(i * part, part)
        values = tok_v[at, :].astype(F32)
        centre = values - jnp.mean(values, axis=-1, keepdims=True)
        spread = jnp.mean(centre * centre, axis=-1, keepdims=True)
        normed[at, :] = (
            centre * lax.rsqrt(spread + 1e-05) * gain_v[...] + bias_v[...]
        ).astype(BF)
    tile = 256
    for s in range(0, rows, tile):
        r = lax.broadcasted_iota(jnp.int32, (tile, n), 0) + s
        hit = (r == place[0]) | (r == place[1])
        buf[s : s + tile, :] = dot(jnp.where(hit, 1.0, 0.0).astype(BF), normed[...]).astype(BF)


PARTS = 4
HOLD = 2900
LAST = 1
HB = pl.BlockSpec(memory_space=pltpu.HBM)
VM = pl.BlockSpec(memory_space=pltpu.VMEM)
CAP = 16
MB = 1024 * 1024


def pack(tokens, gain, bias, ids, weight, rows):
    n, width = tokens.shape
    return pl.pallas_call(
        pack_kernel,
        in_specs=[HB] * 5,
        out_specs=[VM] * 2,
        out_shape=[
            jax.ShapeDtypeStruct((rows, width), BF),
            jax.ShapeDtypeStruct((n, rows), BF),
        ],
        scratch_shapes=[
            pltpu.VMEM((n, width), BF),
            pltpu.VMEM((1, width), F32),
            pltpu.VMEM((1, width), F32),
            pltpu.VMEM((2, n), jnp.int32),
            pltpu.VMEM((2, n), F32),
            pltpu.VMEM((n, width), BF),
            pltpu.VMEM((8, n), F32),
            pltpu.SMEM((1,), jnp.int32),
            pltpu.SemaphoreType.DMA((4 + PARTS,)),
        ],
        compiler_params=pltpu.CompilerParams(vmem_limit_bytes=14 * MB),
        name="pack",
    )(*[stay(a) for a in (tokens, gain.reshape(1, -1), bias.reshape(1, -1), ids.T, weight.T)])


def expert_kernel(x, ga, gb, ua, ub, da, db, mark, out):
    tile = 256
    for s in range(0, x.shape[0], tile):
        rows = x[s : s + tile, :]
        total = None
        for g, u, d in ((ga, ua, da), (gb, ub, db)):
            gate = dot(rows, g[...])
            hidden = (gate / (1.0 + jnp.exp(-gate)) * dot(rows, u[...])).astype(BF)
            part = dot(hidden, d[...])
            total = part if total is None else total + part
        out[s : s + tile, :] = total.astype(BF)


def expert(x, weights, mark):
    rows, width = x.shape
    return pl.pallas_call(
        expert_kernel,
        in_specs=[VM] * 8,
        out_specs=VM,
        out_shape=jax.ShapeDtypeStruct((rows, width), BF),
        compiler_params=pltpu.CompilerParams(vmem_limit_bytes=28 * MB),
        name="expert",
    )(x, *weights, mark)


def mix_kernel(ret, ids_t, weight_t, early_pick, out, side, pick, done, sems):
    rows = ret.shape[0]
    _, width = out.shape

    @pl.when(lax.axis_index("tp") == LAST)
    def _():
        pick[...] = early_pick[...]

    @pl.when(lax.axis_index("tp") != LAST)
    def _():
        picks(place_rows(ids_t[...], rows // CAP, CAP), weight_t, side, pick)

    for i in range(TILES):
        at = pl.ds(i * (width // TILES), width // TILES)
        done[:, at] = dot(pick[...], ret[:, at]).astype(BF)
        pltpu.make_async_copy(done.at[:, at], out.at[:, at], sems.at[i]).start()
    for i in range(TILES):
        at = pl.ds(i * (width // TILES), width // TILES)
        pltpu.make_async_copy(done.at[:, at], out.at[:, at], sems.at[i]).wait()


TILES = 4


def mix(ret, ids, weight, pick):
    n = ids.shape[0]
    rows, width = ret.shape
    return pl.pallas_call(
        mix_kernel,
        in_specs=[VM] * 4,
        out_specs=HB,
        out_shape=jax.ShapeDtypeStruct((n, width), BF),
        scratch_shapes=[
            pltpu.VMEM((8, n), F32),
            pltpu.VMEM((n, rows), BF),
            pltpu.VMEM((n, width), BF),
            pltpu.SemaphoreType.DMA((TILES,)),
        ],
        compiler_params=pltpu.CompilerParams(vmem_limit_bytes=14 * MB),
        name="mix",
    )(ret, ids.T, weight.T, pick)


def body(
    tokens, norm_gain, norm_bias, gate_weight, up_weight, down_weight, expert_ids, route_weights
):
    width = tokens.shape[1]
    experts = lax.axis_size("ep")
    swap = [(0, 1), (1, 0)]
    weights = []
    for w in (gate_weight[0], up_weight[0], down_weight[0]):
        weights += [w, lax.ppermute(w, "tp", swap)]
    buffer, pick = pack(
        tokens, norm_gain, norm_bias, expert_ids, route_weights, experts * CAP
    )
    rows = lax.all_to_all(
        buffer.reshape(experts, CAP, width), "ep", split_axis=0, concat_axis=0, tiled=True
    ).reshape(-1, width)
    mark = rows[:16, :128] * 2
    result = expert(rows, weights, mark)
    returned = lax.all_to_all(
        result.reshape(experts, CAP, width), "ep", split_axis=0, concat_axis=0, tiled=True
    )
    return mix(returned.reshape(-1, width), expert_ids, route_weights, pick)


def solution(mesh):
    placed = (
        P(("ep", "tp"), None),
        P(),
        P(),
        P("ep", None, "tp"),
        P("ep", None, "tp"),
        P("ep", "tp", None),
        P(("ep", "tp"), None),
        P(("ep", "tp"), None),
    )
    return jax.shard_map(
        body, mesh=mesh, in_specs=placed, out_specs=P(("ep", "tp"), None), check_vma=False
    )
```

```python
import jax
import jax.numpy as jnp
from jax import lax
from jax.experimental import pallas as pl
from jax.experimental.pallas import tpu as pltpu
from jax.sharding import PartitionSpec as P


BF = jnp.bfloat16
F32 = jnp.float32


def dot(a, b):
    return jnp.dot(a, b, preferred_element_type=F32)


def place_rows(ids_t, experts, capacity):
    n = ids_t.shape[1]
    i = lax.broadcasted_iota(jnp.int32, (n, n), 0)
    j = lax.broadcasted_iota(jnp.int32, (n, n), 1)
    e = lax.broadcasted_iota(jnp.int32, (experts, n), 0)
    one = [(e == ids_t[k : k + 1, :]).astype(F32) for k in range(2)]
    seen = dot((one[0] + one[1]).astype(BF), (i < j).astype(BF))
    slots = [jnp.sum(seen * o, axis=0, keepdims=True).astype(jnp.int32) for o in one]
    return [ids_t[k : k + 1, :] * capacity + slots[k] for k in range(2)]


def picks(place, weight_t, side, pick):
    side[...] = jnp.zeros(side.shape, F32)
    for k in range(2):
        side[k : k + 1, :] = place[k].astype(F32)
        side[2 + k : 3 + k, :] = weight_t[k : k + 1, :]
    cols = side[...].T
    r = lax.broadcasted_iota(jnp.int32, pick.shape, 1)
    hit = [r == cols[:, k : k + 1].astype(jnp.int32) for k in range(2)]
    pick[...] = jnp.where(
        hit[0], cols[:, 2:3], jnp.where(hit[1], cols[:, 3:4], 0.0)
    ).astype(BF)


def stay(a):
    return pltpu.with_memory_space_constraint(a, pltpu.HBM)


def pack_kernel(
    tok, gain, bias, ids_t, weight_t, buf, pick,
    tok_v, gain_v, bias_v, ids_v, weight_v, normed, side, ticks, sems,
):
    n, _ = tok.shape
    rows = buf.shape[0]
    part = n // PARTS
    small = [
        pltpu.make_async_copy(src, dst, sems.at[i])
        for i, (src, dst) in enumerate(
            ((ids_t, ids_v), (gain, gain_v), (bias, bias_v), (weight_t, weight_v))
        )
    ]
    large = [
        pltpu.make_async_copy(
            tok.at[pl.ds(i * part, part)], tok_v.at[pl.ds(i * part, part)], sems.at[4 + i]
        )
        for i in range(PARTS)
    ]
    for copy in small + large:
        copy.start()
    small[0].wait()
    small[3].wait()
    place = place_rows(ids_v[...], rows // CAP, CAP)

    @pl.when(lax.axis_index("tp") == LAST)
    def _():
        picks(place, weight_v, side, pick)
        ticks[0] = 0

        def tick(i, carry):
            ticks[0] = ticks[0] + i
            return carry

        lax.fori_loop(0, HOLD, tick, 0)

    small[1].wait()
    small[2].wait()
    for i in range(PARTS):
        large[i].wait()
        at = pl.ds(i * part, part)
        values = tok_v[at, :].astype(F32)
        centre = values - jnp.mean(values, axis=-1, keepdims=True)
        spread = jnp.mean(centre * centre, axis=-1, keepdims=True)
        normed[at, :] = (
            centre * lax.rsqrt(spread + 1e-05) * gain_v[...] + bias_v[...]
        ).astype(BF)
    tile = 256
    for s in range(0, rows, tile):
        r = lax.broadcasted_iota(jnp.int32, (tile, n), 0) + s
        hit = (r == place[0]) | (r == place[1])
        buf[s : s + tile, :] = dot(jnp.where(hit, 1.0, 0.0).astype(BF), normed[...]).astype(BF)


PARTS = 2
HOLD = 2820
LAST = 1
HB = pl.BlockSpec(memory_space=pltpu.HBM)
VM = pl.BlockSpec(memory_space=pltpu.VMEM)
CAP = 16
MB = 1024 * 1024


def pack(tokens, gain, bias, ids, weight, rows):
    n, width = tokens.shape
    return pl.pallas_call(
        pack_kernel,
        in_specs=[HB] * 5,
        out_specs=[VM] * 2,
        out_shape=[
            jax.ShapeDtypeStruct((rows, width), BF),
            jax.ShapeDtypeStruct((n, rows), BF),
        ],
        scratch_shapes=[
            pltpu.VMEM((n, width), BF),
            pltpu.VMEM((1, width), F32),
            pltpu.VMEM((1, width), F32),
            pltpu.VMEM((2, n), jnp.int32),
            pltpu.VMEM((2, n), F32),
            pltpu.VMEM((n, width), BF),
            pltpu.VMEM((8, n), F32),
            pltpu.SMEM((1,), jnp.int32),
            pltpu.SemaphoreType.DMA((4 + PARTS,)),
        ],
        compiler_params=pltpu.CompilerParams(vmem_limit_bytes=14 * MB),
        name="pack",
    )(*[stay(a) for a in (tokens, gain.reshape(1, -1), bias.reshape(1, -1), ids.T, weight.T)])


def expert_kernel(x, ga, gb, ua, ub, da, db, mark, out):
    tile = 256
    for s in range(0, x.shape[0], tile):
        rows = x[s : s + tile, :]
        total = None
        for g, u, d in ((ga, ua, da), (gb, ub, db)):
            gate = dot(rows, g[...])
            hidden = (gate / (1.0 + jnp.exp(-gate)) * dot(rows, u[...])).astype(BF)
            part = dot(hidden, d[...])
            total = part if total is None else total + part
        out[s : s + tile, :] = total.astype(BF)


def expert(x, weights, mark):
    rows, width = x.shape
    return pl.pallas_call(
        expert_kernel,
        in_specs=[VM] * 8,
        out_specs=VM,
        out_shape=jax.ShapeDtypeStruct((rows, width), BF),
        compiler_params=pltpu.CompilerParams(vmem_limit_bytes=28 * MB),
        name="expert",
    )(x, *weights, mark)


def mix_kernel(ret, ids_t, weight_t, early_pick, out, side, pick, done, sems):
    rows = ret.shape[0]
    _, width = out.shape

    @pl.when(lax.axis_index("tp") == LAST)
    def _():
        pick[...] = early_pick[...]

    @pl.when(lax.axis_index("tp") != LAST)
    def _():
        picks(place_rows(ids_t[...], rows // CAP, CAP), weight_t, side, pick)

    for i in range(TILES):
        at = pl.ds(i * (width // TILES), width // TILES)
        done[:, at] = dot(pick[...], ret[:, at]).astype(BF)
        pltpu.make_async_copy(done.at[:, at], out.at[:, at], sems.at[i]).start()
    for i in range(TILES):
        at = pl.ds(i * (width // TILES), width // TILES)
        pltpu.make_async_copy(done.at[:, at], out.at[:, at], sems.at[i]).wait()


TILES = 2


def mix(ret, ids, weight, pick):
    n = ids.shape[0]
    rows, width = ret.shape
    return pl.pallas_call(
        mix_kernel,
        in_specs=[VM] * 4,
        out_specs=HB,
        out_shape=jax.ShapeDtypeStruct((n, width), BF),
        scratch_shapes=[
            pltpu.VMEM((8, n), F32),
            pltpu.VMEM((n, rows), BF),
            pltpu.VMEM((n, width), BF),
            pltpu.SemaphoreType.DMA((TILES,)),
        ],
        compiler_params=pltpu.CompilerParams(vmem_limit_bytes=14 * MB),
        name="mix",
    )(ret, ids.T, weight.T, pick)


def body(
    tokens, norm_gain, norm_bias, gate_weight, up_weight, down_weight, expert_ids, route_weights
):
    width = tokens.shape[1]
    experts = lax.axis_size("ep")
    swap = [(0, 1), (1, 0)]
    weights = []
    for w in (gate_weight[0], up_weight[0], down_weight[0]):
        weights += [w, lax.ppermute(w, "tp", swap)]
    buffer, pick = pack(
        tokens, norm_gain, norm_bias, expert_ids, route_weights, experts * CAP
    )
    rows = lax.all_to_all(
        buffer.reshape(experts, CAP, width), "ep", split_axis=0, concat_axis=0, tiled=True
    ).reshape(-1, width)
    mark = rows[:16, :128] * 2
    result = expert(rows, weights, mark)
    returned = lax.all_to_all(
        result.reshape(experts, CAP, width), "ep", split_axis=0, concat_axis=0, tiled=True
    )
    return mix(returned.reshape(-1, width), expert_ids, route_weights, pick)


def solution(mesh):
    placed = (
        P(("ep", "tp"), None),
        P(),
        P(),
        P("ep", None, "tp"),
        P("ep", None, "tp"),
        P("ep", "tp", None),
        P(("ep", "tp"), None),
        P(("ep", "tp"), None),
    )
    return jax.shard_map(
        body, mesh=mesh, in_specs=placed, out_specs=P(("ep", "tp"), None), check_vma=False
    )
```
